32 devices in a mesh: sp: 8 (over z, x), tp: 4 (over y, core).
Axes of the slice: x: 2, y: 2, z: 4, core: 2. Of those that a mesh axis runs over, the one named last changes fastest.
Arguments:
- tokens: bfloat16 [4096, 4096], P('sp'), may hold values from -6 to 6
- norm_gain: float32 [4096], replicated, may hold values from 0.1 to 1.9
- w_pool_in: bfloat16 [4096, 2048], P(None, 'tp'), may hold values from -0.09375 to 0.09375
- w_query: bfloat16 [4096, 2048], P(None, 'tp'), may hold values from -0.15625 to 0.15625
- w_key: bfloat16 [4096, 2048], P(None, 'tp'), may hold values from -0.15625 to 0.15625
- w_value: bfloat16 [4096, 2048], P(None, 'tp'), may hold values from -0.09375 to 0.09375
- pool_mix: bfloat16 [32, 64, 64], P('tp'), may hold values from -0.75 to 0.75
- pool_scale: float32 [2048], P('tp'), may hold values from 0.1 to 1.9
- lam: float32 [16], P('tp'), may hold values from 0.3 to 0.8
- head_gain: float32 [128], replicated, may hold values from 0.1 to 1.9
- pool_proj: bfloat16 [2048, 4096], P('tp'), may hold values from -0.125 to 0.125
- attn_proj: bfloat16 [2048, 4096], P('tp'), may hold values from -0.125 to 0.125
Outputs:
- mixed: bfloat16 [4096, 4096], P(('sp', 'tp'))
The draws below stay inside these ranges and needn't reach their ends.
All inputs are finite; a program needn't handle non-finite values.
Results may differ from the reference program's by a relative error of at most 0.015.
Values may be sent and summed in bfloat16 or wider, within the bound.
A program may use at most 128 MiB of HBM per device.

```python
import jax
import jax.numpy as jnp
from jax import lax

D = 4096
GROUPS = 32
GDIM = 64
HEADS = 16
HEAD = 64
VDIM = 128
SEGMENT = 64
REACH = 16
POOL = 2048
TOKENS = 4096
N_TP = 4


def weight_noise(key, stream_id):
    drawn = 1.3 * jax.random.normal(jax.random.fold_in(key, stream_id), (D, HEADS * 2 * HEAD), jnp.float32)
    return jnp.clip(drawn, -7.8, 7.8) * D ** (-0.5)


def draw_tokens(key, part):
    noise_key = jax.random.fold_in(key, 11)
    drawn = jax.random.normal(noise_key, (TOKENS, D), jnp.float32)
    return jnp.clip(drawn, -6.0, 6.0).astype(jnp.bfloat16)


def draw_w_query(key, part):
    noise_part = weight_noise(key, 21)
    drawn = noise_part
    return drawn.astype(jnp.bfloat16)


def draw_w_key(key, part):
    noise_part = weight_noise(key, 22)
    drawn = noise_part
    return drawn.astype(jnp.bfloat16)


def shard_levels(rng, shape, split, smallest, largest):
    level = 1.0
    for axis_at, shards_of in split:
        heights = jax.random.uniform(jax.random.fold_in(jax.random.fold_in(rng, 6), axis_at), (shards_of,), jnp.float32, smallest / len(split), largest / len(split))
        level = level * jnp.repeat(jnp.exp(heights), shape[axis_at] // shards_of).reshape((-1,) + (1,) * (len(shape) - 1 - axis_at))
    return level


def scatter_about(rng, extent, deviation, most, pieces=(), kind=jnp.bfloat16):
    factor_of = shard_levels(rng, extent, pieces, -0.22, 0.18) if pieces else 1.0
    values = jax.random.normal(rng, extent, jnp.float32) * deviation * factor_of
    return jnp.minimum(jnp.maximum(values, -most), most).astype(kind)


def setup_inputs(seed: int = 0) -> dict:
    splits = jax.random.split(jax.random.key(seed), 13)
    tokens = draw_tokens(jax.random.fold_in(splits[12], 71), 0)
    norm_gain = jnp.clip(1.0 + 0.18 * jax.random.normal(splits[1], (D,), jnp.float32), 0.1, 1.9)
    w_pool_in = scatter_about(splits[2], (D, POOL), D ** -0.5, 0.09375, ((1, 4),))
    w_query = draw_w_query(jax.random.fold_in(splits[12], 71), 0)
    w_key = draw_w_key(jax.random.fold_in(splits[12], 71), 0)
    w_value = scatter_about(splits[5], (D, HEADS * VDIM), D ** -0.5, 0.09375, ((1, 4),))
    pool_mix = scatter_about(splits[6], (GROUPS, GDIM, GDIM), GDIM ** -0.5, 0.75, ((0, 4),))
    pool_scale = jnp.clip(1.0 + 0.18 * jax.random.normal(splits[7], (POOL,), jnp.float32), 0.1, 1.9)
    lam = jnp.clip(0.3 + 0.5 * jax.random.uniform(splits[8], (HEADS,), jnp.float32) ** shard_levels(splits[8], (HEADS,), ((0, 4),), -0.2, 0.2), 0.3, 0.8)
    head_gain = jnp.clip(1.0 + 0.18 * jax.random.normal(splits[9], (VDIM,), jnp.float32), 0.1, 1.9)
    pool_proj = scatter_about(splits[10], (POOL, D), POOL ** -0.5, 0.125, ((0, 4),))
    attn_proj = scatter_about(splits[11], (HEADS * VDIM, D), (HEADS * VDIM) ** -0.5, 0.125, ((0, 4),))
    return {"tokens": tokens, "norm_gain": norm_gain, "w_pool_in": w_pool_in, "w_query": w_query, "w_key": w_key, "w_value": w_value, "pool_mix": pool_mix, "pool_scale": pool_scale, "lam": lam, "head_gain": head_gain, "pool_proj": pool_proj, "attn_proj": attn_proj}


eps_norm = 1e-06
neg_big = -1e+30
out_scale = 0.8

def reference(tokens, norm_gain, w_pool_in, w_query, w_key, w_value, pool_mix, pool_scale, lam, head_gain, pool_proj, attn_proj):
    wide = tokens.astype(jnp.float32)
    normed = (wide * lax.rsqrt(lax.optimization_barrier(jnp.mean(wide * wide, axis=-1, keepdims=True)) + eps_norm) * norm_gain).astype(jnp.bfloat16)
    pool_in = jnp.dot(normed, w_pool_in, preferred_element_type=jnp.float32).astype(jnp.bfloat16)
    query = jnp.dot(normed, w_query, preferred_element_type=jnp.float32).astype(jnp.bfloat16)
    keys = jnp.dot(normed, w_key, preferred_element_type=jnp.float32).astype(jnp.bfloat16)
    values = jnp.dot(normed, w_value, preferred_element_type=jnp.float32).astype(jnp.bfloat16)
    padded = jnp.concatenate([jnp.zeros((REACH - 1, POOL), jnp.float32), pool_in.astype(jnp.float32)], 0)
    channel_group = jnp.arange(POOL, dtype=jnp.int32) // GDIM
    window = 2 ** (1 + channel_group % 4)
    total = jnp.zeros((TOKENS, POOL), jnp.float32)
    for back in range(REACH):
        low = REACH - 1 - back
        total = total + jnp.where(back < window[None, :], padded[low:low + TOKENS], 0.0)
    position = jnp.arange(TOKENS, dtype=jnp.int32)
    count = jnp.minimum(position[:, None] + 1, window[None, :]).astype(jnp.float32)
    pooled = (total / count - pool_in.astype(jnp.float32)).astype(jnp.bfloat16)
    grouped = jnp.einsum('sgi,gio->sgo', pooled.reshape(TOKENS, GROUPS, GDIM).astype(jnp.float32), pool_mix.astype(jnp.float32))
    pool_out = (grouped.reshape(TOKENS, POOL) * pool_scale).astype(jnp.bfloat16)
    query_heads = query.reshape(TOKENS, HEADS, 2, HEAD).transpose(1, 0, 2, 3)
    key_heads = keys.reshape(TOKENS, HEADS, 2, HEAD).transpose(1, 0, 2, 3)
    value_heads = values.reshape(TOKENS, HEADS, VDIM).transpose(1, 0, 2)
    segments = position // SEGMENT
    block = min(TOKENS, 512) if TOKENS % min(TOKENS, 512) == 0 else TOKENS
    scale = HEAD ** (-0.5)

    def one_head(args):
        query_head, key_head, value_head, lam_head = args

        def one_block(index):
            first = (index * block).astype(jnp.int32)
            query_block = lax.dynamic_slice_in_dim(query_head, first, block, 0)
            query_seg = (first + jnp.arange(block, dtype=jnp.int32)) // SEGMENT
            allowed = segments[None, :] <= query_seg[:, None]
            results = []
            for which in range(2):
                scores = jnp.dot(query_block[:, which], key_head[:, which].T, preferred_element_type=jnp.float32) * scale
                masked = jnp.where(allowed, scores, neg_big)
                top = lax.optimization_barrier(jnp.max(masked, axis=-1, keepdims=True))
                probs = jnp.where(allowed, jnp.exp(masked - top), 0.0)
                weighted = jnp.dot(probs.astype(jnp.bfloat16), value_head, preferred_element_type=jnp.float32)
                results.append(weighted / lax.optimization_barrier(jnp.sum(probs, axis=-1, keepdims=True)))
            blend = results[0] - lam_head * results[1]
            scaled = blend * lax.rsqrt(lax.optimization_barrier(jnp.mean(blend * blend, axis=-1, keepdims=True)) + eps_norm) * head_gain * out_scale
            return scaled.astype(jnp.bfloat16)
        return lax.map(one_block, jnp.arange(TOKENS // block, dtype=jnp.int32))
    per_head = lax.map(one_head, (query_heads, key_heads, value_heads, lam))
    attn_out = per_head.reshape(HEADS, TOKENS, VDIM).transpose(1, 0, 2).reshape(TOKENS, HEADS * VDIM)
    pool_share = POOL // N_TP
    attn_share = HEADS * VDIM // N_TP
    summed = jnp.zeros((TOKENS, D), jnp.float32)
    for part in range(N_TP):
        term = jnp.dot(pool_out[:, part * pool_share:(part + 1) * pool_share], pool_proj[part * pool_share:(part + 1) * pool_share], preferred_element_type=jnp.float32)
        term = term + jnp.dot(attn_out[:, part * attn_share:(part + 1) * attn_share], attn_proj[part * attn_share:(part + 1) * attn_share], preferred_element_type=jnp.float32)
        summed = summed + lax.optimization_barrier(term.astype(jnp.bfloat16)).astype(jnp.float32)
    return summed.astype(jnp.bfloat16)
```

```python
import functools

import jax
import jax.numpy as jnp
from jax import lax
from jax.experimental import pallas as pl
from jax.experimental.pallas import tpu as pltpu
from jax.sharding import PartitionSpec as P

GDIM = 64
HEAD = 64
VDIM = 128
SEGMENT = 64
REACH = 16
CHUNK = 256

eps_norm = 1e-06
neg_big = -1e30
out_scale = 0.8
log2_e = 1.4426950408889634


def normalize(rows_in, gain):
    wide = rows_in.astype(jnp.float32)
    scaled = wide * lax.rsqrt(jnp.mean(wide * wide, axis=-1, keepdims=True) + eps_norm) * gain
    return scaled.astype(jnp.bfloat16)


def pool_kernel(x_ref, rim_ref, mix_ref, scale_ref, out_ref):
    rows, width = x_ref.shape
    x = x_ref[...].astype(jnp.float32)
    padded = jnp.concatenate([rim_ref[...].astype(jnp.float32), x], 0)
    group = lax.axis_index("tp") * (width // GDIM) + lax.broadcasted_iota(
        jnp.int32, (1, width), 1
    ) // GDIM
    window = 2 << (group % 4)
    running = padded
    total = jnp.zeros_like(padded)
    for level in range(4):
        running = running + pltpu.roll(running, 1 << level, 0)
        total = jnp.where(group % 4 == level, running, total)
    position = lax.axis_index("sp") * rows + lax.broadcasted_iota(jnp.int32, (rows, 1), 0)
    count = jnp.minimum(position + 1, window).astype(jnp.float32)
    pooled = (total[REACH:] / count - x).astype(jnp.bfloat16)
    for pair in range(width // 128):
        cols = slice(pair * 128, pair * 128 + 128)
        mixed = jnp.dot(pooled[:, cols], mix_ref[pair], preferred_element_type=jnp.float32)
        out_ref[:, cols] = (mixed * scale_ref[:, cols]).astype(jnp.bfloat16)


def pooling(pool_in, rim, pool_mix, pool_scale):
    groups = pool_mix.shape[0]
    pairs = pool_mix.reshape(groups // 2, 2, GDIM, GDIM)
    zero = jnp.zeros_like(pairs[:, 0])
    mix = jnp.concatenate(
        [
            jnp.concatenate([pairs[:, 0], zero], 2),
            jnp.concatenate([zero, pairs[:, 1]], 2),
        ],
        1,
    )
    rows, width = pool_in.shape
    return pl.pallas_call(
        pool_kernel,
        out_shape=jax.ShapeDtypeStruct((rows, width), jnp.bfloat16),
        cost_estimate=pl.CostEstimate(
            flops=rows * width * 256, bytes_accessed=4 * rows * width, transcendentals=0
        ),
        name="pooling",
    )(pool_in, rim, mix, pool_scale.reshape(1, width))


def attend_kernel(lam_ref, k_ref, v_ref, q_ref, gain_ref, out_ref, turned, stacked, peak, total, acc):
    parts, rows = k_ref.shape[:2]
    sub = out_ref.shape[1]
    chunk = min(CHUNK, 2 * sub)
    step = pl.program_id(0)
    share = rows // sub
    mine = lax.axis_index("sp")
    head, place = mine // share, mine % share

    @pl.when(step == 0)
    def _():
        @pl.loop(0, parts)
        def _(index):
            turned[index] = v_ref[index].T

    query = q_ref[step]
    lane = lax.broadcasted_iota(jnp.int32, query.shape, 1)
    stacked[:sub] = jnp.where(lane < HEAD, query, 0)
    stacked[sub:] = jnp.where(lane < HEAD, 0, query)

    def block(index, first):
        k = k_ref[index]
        v = turned[index]
        for start in range(0, 2 * sub, chunk):
            cols = slice(start, start + chunk)
            scores = lax.dot_general(
                k, stacked[cols], (((1,), (1,)), ((), ())), preferred_element_type=jnp.float32
            )
            if first:
                key_seg = lax.broadcasted_iota(jnp.int32, (rows, 1), 0) // SEGMENT
                query_at = (start + lax.broadcasted_iota(jnp.int32, (1, chunk), 1)) % sub
                query_seg = (place * sub + query_at) // SEGMENT
                scores = jnp.where(key_seg <= query_seg, scores, neg_big)
                top = jnp.max(scores, axis=0, keepdims=True)
            else:
                old = peak[:, cols]
                top = jnp.maximum(old, jnp.max(scores, axis=0, keepdims=True))
                shrink = jnp.exp2(old - top)
            probs = jnp.exp2(scores - top)
            summed = jnp.sum(probs, axis=0, keepdims=True)
            weighted = jnp.dot(v, probs.astype(jnp.bfloat16), preferred_element_type=jnp.float32)
            peak[:, cols] = top
            if first:
                total[:, cols] = summed
                acc[:, cols] = weighted
            else:
                total[:, cols] = total[:, cols] * shrink + summed
                acc[:, cols] = acc[:, cols] * shrink + weighted

    block(step, True)

    @pl.loop(0, step)
    def _(index):
        block(index, False)

    averaged = acc[...] / total[...]
    blend = averaged[:, :sub] - lam_ref[head] * averaged[:, sub:]
    scaled = blend * lax.rsqrt(jnp.mean(blend * blend, axis=0, keepdims=True) + eps_norm)
    out_ref[0] = (scaled.T * gain_ref[...] * out_scale).astype(jnp.bfloat16)


def attend(query, keys, values, lam, head_gain):
    rows, width = query.shape
    heads = width // VDIM
    parts = lax.axis_size("sp")
    share = parts // heads
    sub = rows // share

    def to_all(array):
        by_head = array.reshape(rows, heads, VDIM).transpose(1, 0, 2)
        copies = jnp.broadcast_to(by_head[:, None], (heads, share, rows, VDIM))
        copies = copies.reshape(parts, rows, VDIM)
        return lax.all_to_all(copies, "sp", 0, 0, tiled=True)

    query = query.reshape(share, sub, heads, VDIM).transpose(2, 0, 1, 3)
    query = query.reshape(parts, sub, VDIM)
    received = (
        to_all(keys),
        to_all(values),
        lax.all_to_all(query, "sp", 0, 0, tiled=True),
    )
    work = rows * rows * parts * parts // share
    out = pl.pallas_call(
        attend_kernel,
        grid=(parts,),
        in_specs=[
            pl.BlockSpec(memory_space=pltpu.SMEM),
            *[pl.BlockSpec(array.shape, lambda i: (0, 0, 0)) for array in received],
            pl.BlockSpec((1, VDIM), lambda i: (0, 0)),
        ],
        out_specs=pl.BlockSpec((1, sub, VDIM), lambda i: (i, 0, 0)),
        out_shape=jax.ShapeDtypeStruct((parts, sub, VDIM), jnp.bfloat16),
        scratch_shapes=[
            pltpu.VMEM((parts, VDIM, rows), jnp.bfloat16),
            pltpu.VMEM((2 * sub, VDIM), jnp.bfloat16),
            pltpu.VMEM((1, 2 * sub), jnp.float32),
            pltpu.VMEM((1, 2 * sub), jnp.float32),
            pltpu.VMEM((VDIM, 2 * sub), jnp.float32),
        ],
        cost_estimate=pl.CostEstimate(
            flops=work * 512, bytes_accessed=6 * received[0].size, transcendentals=work
        ),
        compiler_params=pltpu.CompilerParams(vmem_limit_bytes=40 * 2**20),
        name="attend",
    )(lam, *received, head_gain.reshape(1, VDIM))
    back = lax.all_to_all(out, "sp", 0, 0, tiled=True)
    back = back.reshape(heads, share, sub, VDIM).transpose(1, 2, 0, 3)
    return back.reshape(rows, width)


MESH = pl.DeviceIdType.MESH


def merge_kernel(tp, pool_ref, attn_ref, wp_ref, wa_ref, out_ref, pairs_out, pairs_in, own, far_out, far_in,
                 pair_send, pair_recv, far_send, far_recv):
    rows, width = pool_ref.shape
    depth = wp_ref.shape[1]
    sides = tp // 2
    piece = rows // tp
    parts, span = pairs_out.shape[1], pairs_out.shape[3]
    me = lax.axis_index("tp")
    side, core = me // 2, me % 2
    mate = side * 2 + 1 - core

    barrier = pltpu.get_barrier_semaphore()
    pl.semaphore_signal(barrier, inc=1, device_id={"tp": mate}, device_id_type=MESH)
    for away in range(1, sides):
        other = ((side + away) % sides) * 2 + core
        pl.semaphore_signal(barrier, inc=1, device_id={"tp": other}, device_id_type=MESH)
    pl.semaphore_wait(barrier, sides)

    def pair_copy(away, part):
        return pltpu.make_async_remote_copy(
            src_ref=pairs_out.at[away, part], dst_ref=pairs_in.at[away, part],
            send_sem=pair_send.at[away, part], recv_sem=pair_recv.at[away, part],
            device_id={"tp": mate}, device_id_type=MESH)

    def far_copy(away, part):
        other = ((side + away) % sides) * 2 + core
        return pltpu.make_async_remote_copy(
            src_ref=far_out.at[away, part], dst_ref=far_in.at[away, part],
            send_sem=far_send.at[away, part], recv_sem=far_recv.at[away, part],
            device_id={"tp": other}, device_id_type=MESH)

    def compute(away, part):
        at = pl.multiple_of(((side + away) % sides) * 2 * piece, 2 * piece)
        cols = pl.ds(pl.multiple_of(part * span, span), span)
        term = jnp.dot(pool_ref[pl.ds(at, 2 * piece)], wp_ref[:, cols], preferred_element_type=jnp.float32)
        term = term + jnp.dot(attn_ref[pl.ds(at, 2 * piece)], wa_ref[:, cols], preferred_element_type=jnp.float32)
        low, high = term[:piece], term[piece:]
        own[away, part] = jnp.where(core == 0, low, high)
        pairs_out[away, part] = jnp.where(core == 0, high, low).astype(jnp.bfloat16)
        pair_copy(away, part).start()

    def combine(away, part):
        pair_copy(away, part).wait_recv()
        return own[away, part] + pairs_in[away, part].astype(jnp.float32)

    units = sides * parts

    @pl.loop(0, units + 1)
    def _(unit):
        @pl.when(unit < units)
        def _():
            compute((unit // parts + 1) % sides, unit % parts)

        @pl.when(unit > 0)
        def _():
            last = unit - 1
            away, part = (last // parts + 1) % sides, last % parts
            both = combine(away, part)

            @pl.when(away != 0)
            def _():
                far_out[away, part] = both.astype(jnp.bfloat16)
                far_copy(away, part).start()

            @pl.when(away == 0)
            def _():
                own[away, part] = both

    for part in range(parts):
        total = own[0, part]
        for away in range(1, sides):
            far_copy(away, part).wait_recv()
            total = total + far_in[away, part].astype(jnp.float32)
        out_ref[:, part * span : part * span + span] = total.astype(jnp.bfloat16)

    @pl.loop(0, units)
    def _(unit):
        pair_copy(unit // parts, unit % parts).wait_send()

    @pl.loop(parts, units)
    def _(unit):
        far_copy(unit // parts, unit % parts).wait_send()


def merge(pool_out, attn_out, pool_proj, attn_proj):
    tp = lax.axis_size("tp")
    rows, width = pool_out.shape
    depth = pool_proj.shape[1]
    span = 1024
    parts = depth // span
    sides, piece = tp // 2, rows // tp
    vmem = pl.BlockSpec(memory_space=pltpu.VMEM)
    return pl.pallas_call(
        functools.partial(merge_kernel, tp),
        out_shape=jax.ShapeDtypeStruct((piece, depth), jnp.bfloat16),
        in_specs=[vmem] * 4,
        out_specs=vmem,
        scratch_shapes=[
            pltpu.VMEM((sides, parts, piece, span), jnp.bfloat16),
            pltpu.VMEM((sides, parts, piece, span), jnp.bfloat16),
            pltpu.VMEM((sides, parts, piece, span), jnp.float32),
            pltpu.VMEM((sides, parts, piece, span), jnp.bfloat16),
            pltpu.VMEM((sides, parts, piece, span), jnp.bfloat16),
            pltpu.SemaphoreType.DMA((sides, parts)),
            pltpu.SemaphoreType.DMA((sides, parts)),
            pltpu.SemaphoreType.DMA((sides, parts)),
            pltpu.SemaphoreType.DMA((sides, parts)),
        ],
        compiler_params=pltpu.CompilerParams(
            collective_id=0, has_side_effects=True, vmem_limit_bytes=48 * 2**20
        ),
        cost_estimate=pl.CostEstimate(
            flops=4 * rows * width * depth, bytes_accessed=4 * width * depth, transcendentals=0
        ),
        name="merge",
    )(pool_out, attn_out, pool_proj, attn_proj)


def body(
    tokens,
    norm_gain,
    w_pool_in,
    w_query,
    w_key,
    w_value,
    pool_mix,
    pool_scale,
    lam,
    head_gain,
    pool_proj,
    attn_proj,
):
    count_rows = tokens.shape[0]
    normed = normalize(tokens, norm_gain)
    keys = jnp.dot(normed, w_key, preferred_element_type=jnp.float32).astype(jnp.bfloat16)
    values = jnp.dot(normed, w_value, preferred_element_type=jnp.float32).astype(jnp.bfloat16)
    pool_in = jnp.dot(normed, w_pool_in, preferred_element_type=jnp.float32).astype(jnp.bfloat16)
    devices = lax.axis_size("sp")
    rim = lax.ppermute(
        pool_in[count_rows - REACH :], "sp", [(i, i + 1) for i in range(devices - 1)]
    )
    query = (
        jnp.dot(normed, w_query, preferred_element_type=jnp.float32) * (HEAD ** (-0.5) * log2_e)
    ).astype(jnp.bfloat16)
    pool_out = pooling(pool_in, rim, pool_mix, pool_scale)
    attn_out = attend(query, keys, values, lam, head_gain)
    return merge(pool_out, attn_out, pool_proj, attn_proj)


def solution(mesh):
    return jax.shard_map(
        body,
        mesh=mesh,
        in_specs=(
            P("sp", None),
            P(),
            P(None, "tp"),
            P(None, "tp"),
            P(None, "tp"),
            P(None, "tp"),
            P("tp", None, None),
            P("tp"),
            P("tp"),
            P(),
            P("tp", None),
            P("tp", None),
        ),
        out_specs=P(("sp", "tp"), None),
        check_vma=False,
    )
```

```python
import functools

import jax
import jax.numpy as jnp
from jax import lax
from jax.experimental import pallas as pl
from jax.experimental.pallas import tpu as pltpu
from jax.sharding import PartitionSpec as P

GDIM = 64
HEAD = 64
VDIM = 128
SEGMENT = 64
REACH = 16
PASSES = 2
SPAN = 1024
SLAB = 256
LOADS = 4
MESH = pl.DeviceIdType.MESH

eps_norm = 1e-06
neg_big = -1e30
out_scale = 0.8
log2_e = 1.4426950408889634


class Shape:
    def __init__(self, sp, tp, rows, depth, width):
        self.sp, self.tp, self.rows, self.depth, self.width = sp, tp, rows, depth, width
        self.heads = width // VDIM
        self.share = sp // self.heads
        self.per = tp // self.share
        self.piece = rows // tp
        self.run = self.piece // PASSES
        self.n = self.per * self.run
        self.cols = 4 * self.n
        self.sides = tp // 2
        self.parts = depth // SPAN
        self.slabs = width // SLAB
        self.slab_heads = SLAB // VDIM


def layer_kernel(z, lam_ref, tok_hbm, gain_ref, wp_hbm, wq_hbm, wk_hbm, wv_hbm, mix_ref, scale_ref, head_gain_ref,
                 pp_hbm, ap_hbm, out_ref,
                 tok, normed, weights, proj, res, k_own, v_own, q_own, k_all, v_all, q_all, lhs, o_own, pool_in, rim,
                 stacked, turned, even, odd, acc, pairs_out, pairs_in, mine, far_out, far_in,
                 tok_sem, w_sem, p_sem, z_send, z_recv, x_send, x_recv, q_send, q_recv, o_send, o_recv,
                 rim_send, rim_recv, pair_send, pair_recv, far_send, far_recv):
    me = lax.axis_index("sp")
    spot = lax.axis_index("tp")
    head, place = me // z.share, me % z.share
    side, core = spot // 2, spot % 2
    mate = side * 2 + 1 - core
    bf16, f32 = jnp.bfloat16, jnp.float32

    def to_sp(src, dst, send, recv, device):
        return pltpu.make_async_remote_copy(
            src_ref=src, dst_ref=dst, send_sem=send, recv_sem=recv,
            device_id={"sp": device}, device_id_type=MESH)

    def to_tp(src, dst, send, recv, device):
        return pltpu.make_async_remote_copy(
            src_ref=src, dst_ref=dst, send_sem=send, recv_sem=recv,
            device_id={"tp": device}, device_id_type=MESH)

    chunk = z.rows // LOADS

    def token_load(i):
        at = pl.ds(pl.multiple_of(i * chunk, chunk), chunk)
        return pltpu.make_async_copy(tok_hbm.at[at], tok.at[at], tok_sem.at[i])

    weight_loads = [
        pltpu.make_async_copy(w, weights.at[i], w_sem.at[i])
        for i, w in enumerate((wk_hbm, wv_hbm, wq_hbm, wp_hbm))
    ]
    proj_loads = [
        pltpu.make_async_copy(w, proj.at[pl.ds(i * z.width, z.width)], p_sem.at[i])
        for i, w in enumerate((pp_hbm, ap_hbm))
    ]
    for i in range(LOADS):
        token_load(i).start()
    for load in weight_loads + proj_loads:
        load.start()

    barrier = pltpu.get_barrier_semaphore()
    for away in range(1, z.sp):
        pl.semaphore_signal(barrier, inc=1, device_id={"sp": (me + away) % z.sp}, device_id_type=MESH)
    pl.semaphore_signal(barrier, inc=1, device_id={"tp": mate}, device_id_type=MESH)
    for away in range(1, z.sides):
        other = ((side + away) % z.sides) * 2 + core
        pl.semaphore_signal(barrier, inc=1, device_id={"tp": other}, device_id_type=MESH)

    @pl.loop(0, LOADS)
    def _(i):
        token_load(i).wait()

        @pl.loop(0, chunk // 32)
        def _(j):
            at = pl.ds(pl.multiple_of(i * chunk + j * 32, 32), 32)
            wide = tok[at].astype(f32)
            scale = lax.rsqrt(jnp.mean(wide * wide, axis=-1, keepdims=True) + eps_norm)
            normed[at] = (wide * scale * gain_ref[...]).astype(bf16)

    pl.semaphore_wait(barrier, z.sp - 1 + z.sides)

    def z_copy(kind, h, source):
        own, all_ = ((k_own, k_all), (v_own, v_all))[kind]
        return to_sp(own.at[h], all_.at[source], z_send.at[kind, h], z_recv.at[kind, source // z.share],
                     h * z.share + place)

    def x_copy(kind, h, source, target):
        all_ = (k_all, v_all)[kind]
        return to_sp(all_.at[source], all_.at[source], x_send.at[kind, h, target],
                     x_recv.at[kind, h, source % z.share], head * z.share + target)

    def spread(h):
        for kind in range(2):
            for away in range(1, z.share):
                x_copy(kind, h, h * z.share + place, (place + away) % z.share).start()

    def send_head(h):
        @pl.when(h == head)
        def _():
            k_all[me] = k_own[h]
            v_all[me] = v_own[h]
            spread(h)

        @pl.when(h != head)
        def _():
            for kind in range(2):
                z_copy(kind, h, me).start()

    def q_copy(a, h, p, source):
        target = h * z.share + p
        return to_sp(q_own.at[h, a, p], q_all.at[a, source], q_send.at[a, target], q_recv.at[a, source], target)

    def rim_copy():
        return to_sp(pool_in.at[pl.ds(z.rows - REACH, REACH)], rim, rim_send, rim_recv, (me + 1) % z.sp)

    first = ((head + z.heads - 1) % z.heads) // z.slab_heads

    for load in weight_loads:
        load.wait()

    @pl.loop(0, 4 * z.slabs)
    def _(u):
        early = u < 2 * z.slabs
        kind = jnp.where(early, u % 2, u // z.slabs)
        step = jnp.where(early, u // 2, u % z.slabs)
        slab = (first + step) % z.slabs
        cols = pl.ds(pl.multiple_of(slab * SLAB, SLAB), SLAB)
        res[...] = jnp.dot(normed[...], weights[kind, :, cols], preferred_element_type=f32)

        @pl.when(kind == 0)
        def _():
            for i in range(z.slab_heads):
                k_own[slab * z.slab_heads + i] = res[:, i * VDIM : i * VDIM + VDIM].astype(bf16)

        @pl.when(kind == 1)
        def _():
            for i in range(z.slab_heads):
                v_own[slab * z.slab_heads + i] = res[:, i * VDIM : i * VDIM + VDIM].astype(bf16).T
            for i in range(z.slab_heads):
                send_head(slab * z.slab_heads + (head + z.heads - 1 - i) % z.slab_heads)

        @pl.when(kind == 2)
        def _():
            for i in range(z.slab_heads):
                for t in range(z.tp):
                    for a in range(PASSES):
                        at = t * z.piece + a * z.run
                        to = (t % z.per) * z.run
                        q_own[slab * z.slab_heads + i, a, t // z.per, to : to + z.run] = (
                            res[at : at + z.run, i * VDIM : i * VDIM + VDIM] * (HEAD ** (-0.5) * log2_e)
                        ).astype(bf16)

            @pl.when(step == z.slabs - 1)
            def _():
                for a in range(PASSES):
                    q_all[a, me] = q_own[head, a, place]
                for a in range(PASSES):
                    for away in range(1, z.sp):
                        target = (me + away) % z.sp
                        q_copy(a, target // z.share, target % z.share, me).start()

        @pl.when(kind == 3)
        def _():
            pool_in[:, cols] = res[...].astype(bf16)

            @pl.when((step == z.slabs - 1) & (me < z.sp - 1))
            def _():
                rim_copy().start()

    for away in range(1, z.heads):
        source = (head + away) % z.heads
        for kind in range(2):
            z_copy(kind, head, source * z.share + place).wait_recv()
        spread(source)

    @pl.when(me == 0)
    def _():
        rim[...] = jnp.zeros_like(rim)

    @pl.when(me > 0)
    def _():
        rim_copy().wait_recv()

    @pl.loop(0, z.width // 128)
    def _(pair):
        cols = pl.ds(pl.multiple_of(pair * 128, 128), 128)
        x = pool_in[:, cols].astype(f32)
        running = jnp.concatenate([rim[:, cols].astype(f32), x], 0)
        group = spot * (z.width // GDIM) + pair * 2 + lax.broadcasted_iota(jnp.int32, (1, 128), 1) // GDIM
        total = jnp.zeros_like(running)
        for level in range(4):
            running = running + pltpu.roll(running, 1 << level, 0)
            total = jnp.where(group % 4 == level, running, total)
        window = 2 << (group % 4)
        position = me * z.rows + lax.broadcasted_iota(jnp.int32, (z.rows, 1), 0)
        count = jnp.minimum(position + 1, window).astype(f32)
        pooled = (total[REACH:] / count - x).astype(bf16)
        mixed = jnp.dot(pooled, mix_ref[pair], preferred_element_type=f32)
        mixed = (mixed * scale_ref[:, cols]).astype(bf16)
        for t in range(z.tp):
            for a in range(PASSES):
                at = t * z.piece + a * z.run
                lhs[a, t * z.run : t * z.run + z.run, cols] = mixed[at : at + z.run]

    for load in proj_loads:
        load.wait()

    def o_copy(a, target, source):
        at = pl.ds(pl.multiple_of((source % z.share) * z.n, z.n), z.n)
        cols = pl.ds(pl.multiple_of(z.width + (source // z.share) * VDIM, VDIM), VDIM)
        return to_sp(o_own.at[a, target], lhs.at[a, at, cols], o_send.at[a, target], o_recv.at[a, source], target)

    def attend(a, duo):
        for j in range(2):
            block = 2 * duo + j

            @pl.when(block != me)
            def _():
                q_copy(a, head, place, block).wait_recv()

            @pl.when((a == 0) & (block % z.share != place))
            def _():
                for kind in range(2):
                    x_copy(kind, block // z.share, block, place).wait_recv()

        lane = lax.broadcasted_iota(jnp.int32, (z.n, VDIM), 1)
        for j in range(2):
            query = q_all[a, 2 * duo + j]
            stacked[2 * j * z.n : (2 * j + 1) * z.n] = jnp.where(lane < HEAD, query, 0)
            stacked[(2 * j + 1) * z.n : (2 * j + 2) * z.n] = jnp.where(lane < HEAD, 0, query)
        turned[...] = stacked[...].T

        def scores(block):
            return jnp.dot(k_all[block], turned[...], preferred_element_type=f32)

        def masked(block):
            key_seg = (block * z.rows + lax.broadcasted_iota(jnp.int32, (z.rows, 1), 0)) // SEGMENT
            col = lax.broadcasted_iota(jnp.int32, (1, z.cols), 1)
            row = col % z.n
            token = (place * z.per + row // z.run) * z.piece + a * z.run + row % z.run
            query_seg = ((2 * duo + col // (2 * z.n)) * z.rows + token) // SEGMENT
            return jnp.where(key_seg <= query_seg, scores(block), neg_big)

        def put(buffer, value):
            buffer[...] = value
            return jnp.max(value, axis=0, keepdims=True)

        def absorb(buffer, top, block, state):
            old, total = state
            new = jnp.maximum(old, top)
            shrink = jnp.exp2(old - new)
            probs = jnp.exp2(buffer[...] - new)
            total = total * shrink + jnp.sum(probs, axis=0, keepdims=True)
            acc[...] = acc[...] * shrink + jnp.dot(v_all[block], probs.astype(bf16), preferred_element_type=f32)
            return new, total

        top_even = put(even, masked(2 * duo))
        top_odd = put(odd, masked(2 * duo + 1))
        probs = jnp.exp2(even[...] - top_even)
        total = jnp.sum(probs, axis=0, keepdims=True)
        acc[...] = jnp.dot(v_all[2 * duo], probs.astype(bf16), preferred_element_type=f32)

        def two(i, carry):
            state, top_odd = carry
            before = jnp.where(i == 0, 2 * duo + 1, 2 * i - 1)
            top_even = put(even, scores(2 * i))
            state = absorb(odd, top_odd, before, state)
            top_odd = put(odd, scores(2 * i + 1))
            state = absorb(even, top_even, 2 * i, state)
            return state, top_odd

        state, top_odd = lax.fori_loop(0, duo, two, ((top_even, total), top_odd))
        _, total = absorb(odd, top_odd, jnp.where(duo == 0, 1, 2 * duo - 1), state)

        averaged = (acc[...] / total).T
        for j in range(2):
            block = 2 * duo + j
            one = averaged[2 * j * z.n : (2 * j + 1) * z.n]
            two_ = averaged[(2 * j + 1) * z.n : (2 * j + 2) * z.n]
            blend = one - lam_ref[head] * two_
            scaled = blend * lax.rsqrt(jnp.mean(blend * blend, axis=-1, keepdims=True) + eps_norm)
            o_own[a, block] = (scaled * head_gain_ref[...] * out_scale).astype(bf16)

            @pl.when(block == me)
            def _():
                at = pl.ds(pl.multiple_of(place * z.n, z.n), z.n)
                cols = pl.ds(pl.multiple_of(z.width + head * VDIM, VDIM), VDIM)
                lhs[a, at, cols] = o_own[a, block]

            @pl.when(block != me)
            def _():
                o_copy(a, block, me).start()

    def pair_copy(a, part):
        return to_tp(pairs_out.at[a, part], pairs_in.at[a, part], pair_send.at[a, part], pair_recv.at[a, part], mate)

    def far_copy(a, away, part):
        other = ((side + away) % z.sides) * 2 + core
        return to_tp(far_out.at[a, away, part], far_in.at[a, away, part], far_send.at[a, away, part],
                     far_recv.at[a, away, part], other)

    def merge(a):
        @pl.loop(1, z.sp)
        def _(away):
            o_copy(a, me, (me + away) % z.sp).wait_recv()

        @pl.loop(0, z.parts + 1)
        def _(part):
            @pl.when(part < z.parts)
            def _():
                cols = pl.ds(pl.multiple_of(part * SPAN, SPAN), SPAN)
                term = jnp.dot(lhs[a], proj[:, cols], preferred_element_type=f32)
                for s in range(z.sides):
                    low = term[2 * s * z.run : (2 * s + 1) * z.run]
                    high = term[(2 * s + 1) * z.run : (2 * s + 2) * z.run]
                    mine[a, part, s] = jnp.where(core == 0, low, high)
                    pairs_out[a, part, s] = jnp.where(core == 0, high, low).astype(bf16)
                pair_copy(a, part).start()

            @pl.when(part > 0)
            def _():
                last = part - 1
                pair_copy(a, last).wait_recv()
                for away in range(1, z.sides):
                    s = (side + away) % z.sides
                    far_out[a, away, last] = (mine[a, last, s] + pairs_in[a, last, s].astype(f32)).astype(bf16)
                    far_copy(a, away, last).start()
                mine[a, last, side] = mine[a, last, side] + pairs_in[a, last, side].astype(f32)

    duos = z.sp // 2
    hold = PASSES * duos - 2

    @pl.loop(0, PASSES * duos + 1)
    def _(it):
        @pl.when(it == hold)
        def _():
            merge(0)

        @pl.when(it < PASSES * duos)
        def _():
            attend(it // duos, it % duos)

        @pl.when(it == PASSES * duos)
        def _():
            merge(1)

    @pl.loop(0, PASSES * z.parts)
    def _(i):
        a, part = i // z.parts, i % z.parts
        total = mine[a, part, side]
        for away in range(1, z.sides):
            far_copy(a, away, part).wait_recv()
            total = total + far_in[a, away, part].astype(f32)
        at = pl.ds(pl.multiple_of(a * z.run, z.run), z.run)
        out_ref[at, pl.ds(pl.multiple_of(part * SPAN, SPAN), SPAN)] = total.astype(bf16)

    for kind in range(2):
        for away in range(1, z.heads):
            z_copy(kind, (head + away) % z.heads, me).wait_send()
        for h in range(z.heads):
            for away in range(1, z.share):
                x_copy(kind, h, h * z.share + place, (place + away) % z.share).wait_send()
    for a in range(PASSES):
        @pl.loop(1, z.sp)
        def _(away):
            target = (me + away) % z.sp
            q_copy(a, target // z.share, target % z.share, me).wait_send()
            o_copy(a, target, me).wait_send()

        @pl.loop(0, z.parts)
        def _(part):
            pair_copy(a, part).wait_send()
            for away in range(1, z.sides):
                far_copy(a, away, part).wait_send()

    @pl.when(me < z.sp - 1)
    def _():
        rim_copy().wait_send()


def body(tokens, norm_gain, w_pool_in, w_query, w_key, w_value, pool_mix, pool_scale, lam, head_gain, pool_proj,
         attn_proj):
    rows, depth = tokens.shape
    width = w_query.shape[1]
    z = Shape(lax.axis_size("sp"), lax.axis_size("tp"), rows, depth, width)
    pairs = pool_mix.reshape(-1, 2, GDIM, GDIM)
    zero = jnp.zeros_like(pairs[:, 0])
    mix = jnp.concatenate(
        [jnp.concatenate([pairs[:, 0], zero], 2), jnp.concatenate([zero, pairs[:, 1]], 2)], 1)
    vmem = pl.BlockSpec(memory_space=pltpu.VMEM)
    hbm = pl.BlockSpec(memory_space=pl.ANY)
    bf16, f32 = jnp.bfloat16, jnp.float32
    dma = pltpu.SemaphoreType.DMA
    scratch = [
        pltpu.VMEM((rows, depth), bf16),
        pltpu.VMEM((rows, depth), bf16),
        pltpu.VMEM((4, depth, width), bf16),
        pltpu.VMEM((2 * width, depth), bf16),
        pltpu.VMEM((rows, SLAB), f32),
        pltpu.VMEM((z.heads, rows, VDIM), bf16),
        pltpu.VMEM((z.heads, VDIM, rows), bf16),
        pltpu.VMEM((z.heads, PASSES, z.share, z.n, VDIM), bf16),
        pltpu.VMEM((z.sp, rows, VDIM), bf16),
        pltpu.VMEM((z.sp, VDIM, rows), bf16),
        pltpu.VMEM((PASSES, z.sp, z.n, VDIM), bf16),
        pltpu.VMEM((PASSES, z.tp * z.run, 2 * width), bf16),
        pltpu.VMEM((PASSES, z.sp, z.n, VDIM), bf16),
        pltpu.VMEM((rows, width), bf16),
        pltpu.VMEM((REACH, width), bf16),
        pltpu.VMEM((z.cols, VDIM), bf16),
        pltpu.VMEM((VDIM, z.cols), bf16),
        pltpu.VMEM((rows, z.cols), f32),
        pltpu.VMEM((rows, z.cols), f32),
        pltpu.VMEM((VDIM, z.cols), f32),
        pltpu.VMEM((PASSES, z.parts, z.sides, z.run, SPAN), bf16),
        pltpu.VMEM((PASSES, z.parts, z.sides, z.run, SPAN), bf16),
        pltpu.VMEM((PASSES, z.parts, z.sides, z.run, SPAN), f32),
        pltpu.VMEM((PASSES, z.sides, z.parts, z.run, SPAN), bf16),
        pltpu.VMEM((PASSES, z.sides, z.parts, z.run, SPAN), bf16),
        dma((LOADS,)), dma((4,)), dma((2,)),
        dma((2, z.heads)), dma((2, z.heads)),
        dma((2, z.heads, z.share)), dma((2, z.heads, z.share)),
        dma((PASSES, z.sp)), dma((PASSES, z.sp)),
        dma((PASSES, z.sp)), dma((PASSES, z.sp)),
        dma, dma,
        dma((PASSES, z.parts)), dma((PASSES, z.parts)),
        dma((PASSES, z.sides, z.parts)), dma((PASSES, z.sides, z.parts)),
    ]
    return pl.pallas_call(
        functools.partial(layer_kernel, z),
        out_shape=jax.ShapeDtypeStruct((rows // z.tp, depth), bf16),
        in_specs=[pl.BlockSpec(memory_space=pltpu.SMEM), hbm, vmem, hbm, hbm, hbm, hbm, vmem, vmem, vmem, hbm, hbm],
        out_specs=vmem,
        scratch_shapes=scratch,
        compiler_params=pltpu.CompilerParams(
            collective_id=0, has_side_effects=True, vmem_limit_bytes=63 * 2**20),
        name="layer",
    )(lam, tokens, norm_gain.reshape(1, depth), w_pool_in, w_query, w_key, w_value, mix,
      pool_scale.reshape(1, width), head_gain.reshape(1, VDIM), pool_proj, attn_proj)


def solution(mesh):
    return jax.shard_map(
        body,
        mesh=mesh,
        in_specs=(
            P("sp", None), P(), P(None, "tp"), P(None, "tp"), P(None, "tp"), P(None, "tp"),
            P("tp", None, None), P("tp"), P("tp"), P(), P("tp", None), P("tp", None),
        ),
        out_specs=P(("sp", "tp"), None),
        check_vma=False,
    )
```

```python
import functools

import jax
import jax.numpy as jnp
from jax import lax
from jax.experimental import pallas as pl
from jax.experimental.pallas import tpu as pltpu
from jax.sharding import PartitionSpec as P

GDIM = 64
HEAD = 64
VDIM = 128
SEGMENT = 64
REACH = 16
PASSES = 2
SPAN = 1024
SLAB = 256
HOLD = 2
ASK = 2
LAG = 2
BAND = 64
LOADS = 4
MESH = pl.DeviceIdType.MESH

eps_norm = 1e-06
neg_big = -1e30
out_scale = 0.8
log2_e = 1.4426950408889634


class Shape:
    def __init__(self, sp, tp, rows, depth, width):
        self.sp, self.tp, self.rows, self.depth, self.width = sp, tp, rows, depth, width
        self.heads = width // VDIM
        self.share = sp // self.heads
        self.per = tp // self.share
        assert self.per in (1, 2) and self.share % 2 == 0
        self.piece = rows // tp
        self.run = self.piece // PASSES
        self.n = self.per * self.run
        self.cols = 4 * self.n
        self.sides = tp // 2
        self.parts = depth // SPAN
        self.slabs = width // SLAB
        self.slab_heads = SLAB // VDIM


def layer_kernel(z, lam_ref, tok_hbm, gain_ref, wp_hbm, wq_hbm, wk_hbm, wv_hbm, mix_ref, scale_ref, head_gain_ref,
                 pp_hbm, ap_hbm, out_ref,
                 tok, weights, proj, res, k_own, v_own, q_own, k_all, v_all, q_all, pool_out, lhs, o_own, pool_in, rim, rim_own,
                 stacked, turned, even, odd, bias, acc, pairs_out, pairs_in, mine, theirs, far_out, far_in,
                 tok_sem, w_sem, p_sem, z_send, z_recv, x_send, x_recv, q_send, q_recv, o_send, o_recv,
                 rim_send, rim_recv, pair_send, pair_recv, far_send, far_recv):
    me = lax.axis_index("sp")
    spot = lax.axis_index("tp")
    head, place = me // z.share, me % z.share
    side, core = spot // 2, spot % 2
    mate = side * 2 + 1 - core
    bf16, f32 = jnp.bfloat16, jnp.float32

    def to_sp(src, dst, send, recv, device):
        return pltpu.make_async_remote_copy(
            src_ref=src, dst_ref=dst, send_sem=send, recv_sem=recv,
            device_id={"sp": device}, device_id_type=MESH)

    def to_tp(src, dst, send, recv, device):
        return pltpu.make_async_remote_copy(
            src_ref=src, dst_ref=dst, send_sem=send, recv_sem=recv,
            device_id={"tp": device}, device_id_type=MESH)

    chunk = z.rows // LOADS

    def token_load(i):
        at = pl.ds(pl.multiple_of(i * chunk, chunk), chunk)
        return pltpu.make_async_copy(tok_hbm.at[at], tok.at[at], tok_sem.at[i])

    weight_loads = [
        pltpu.make_async_copy(w, weights.at[i], w_sem.at[i])
        for i, w in enumerate((wq_hbm, wk_hbm, wv_hbm, wp_hbm))
    ]
    proj_loads = [
        pltpu.make_async_copy(w, proj.at[pl.ds(i * z.width, z.width)], p_sem.at[i])
        for i, w in enumerate((pp_hbm, ap_hbm))
    ]
    for i in range(LOADS):
        token_load(i).start()

    barrier = pltpu.get_barrier_semaphore()
    for away in range(1, z.sp):
        pl.semaphore_signal(barrier, inc=1, device_id={"sp": (me + away) % z.sp}, device_id_type=MESH)
    pl.semaphore_signal(barrier, inc=1, device_id={"tp": mate}, device_id_type=MESH)
    for away in range(1, z.sides):
        other = ((side + away) % z.sides) * 2 + core
        pl.semaphore_signal(barrier, inc=1, device_id={"tp": other}, device_id_type=MESH)

    @pl.loop(0, LOADS)
    @jax.named_scope('norm')
    def _(i):
        token_load(i).wait()
        for at in range(4):
            @pl.when(i == (3, 0, 2, 3)[at])
            def _():
                weight_loads[at].start()

        @pl.loop(0, chunk // BAND)
        def _(j):
            at = pl.ds(pl.multiple_of(i * chunk + j * BAND, BAND), BAND)
            total = jnp.zeros((BAND, 128), f32)
            for c in range(0, z.depth, 128):
                wide = tok[at, c : c + 128].astype(f32)
                total = total + wide * wide
            scale = lax.rsqrt(jnp.sum(total, axis=-1, keepdims=True) * (1.0 / z.depth) + eps_norm)
            scale = jnp.broadcast_to(scale, (BAND, 128))
            for c in range(0, z.depth, 128):
                wide = tok[at, c : c + 128].astype(f32)
                tok[at, c : c + 128] = (wide * scale * gain_ref[:, c : c + 128]).astype(bf16)

    def z_copy(kind, h, source):
        own, all_ = ((k_own, k_all), (v_own, v_all))[kind]
        return to_sp(own.at[h], all_.at[source], z_send.at[kind, h], z_recv.at[kind, source // z.share],
                     h * z.share + place)

    def x_copy(kind, h, source, target):
        all_ = (k_all, v_all)[kind]
        return to_sp(all_.at[source], all_.at[source], x_send.at[kind, h, target],
                     x_recv.at[kind, h, source % z.share], head * z.share + target)

    def spread(kind, h):
        for away in range(1, z.share):
            x_copy(kind, h, h * z.share + place, (place + away) % z.share).start()

    def send_head(h):
        @pl.when(h == head)
        def _():
            k_all[me] = k_own[h]
            v_all[me] = v_own[h]
            for kind in range(2):
                spread(kind, h)

        @pl.when(h != head)
        def _():
            for kind in range(2):
                z_copy(kind, h, me).start()

    def q_copy(a, h, p, source):
        target = h * z.share + p
        return to_sp(q_own.at[h, a, p], q_all.at[a, source], q_send.at[a, target], q_recv.at[a, source], target)

    def send_queries(a):
        @pl.loop(1, z.sp)
        def _(away):
            target = (me + away) % z.sp
            q_copy(a, target // z.share, target % z.share, me).start()

    def rim_copy():
        return to_sp(rim_own, rim, rim_send, rim_recv, (me + 1) % z.sp)

    upper = head >= z.heads // 2

    def project(kind, slab):
        cols = pl.ds(pl.multiple_of(slab * SLAB, SLAB), SLAB)
        return jnp.dot(tok[...], weights[kind, :, cols], preferred_element_type=f32)

    def keep_keys(slab):
        for i in range(z.slab_heads):
            k_own[slab * z.slab_heads + i] = res[:, i * VDIM : i * VDIM + VDIM].astype(bf16)

    def keep_values(slab):
        for i in range(z.slab_heads):
            v_own[slab * z.slab_heads + i] = res[:, i * VDIM : i * VDIM + VDIM].astype(bf16).T

    half = z.heads // 2

    def mirror(h):
        return jnp.where(upper, z.heads - 1 - h, h)

    inner = mirror(head)

    def other_far(j):
        return mirror(half + j + jnp.where(half + j >= z.heads - 1 - inner, 1, 0))

    far = jnp.where(upper, 0, z.slabs - 1)

    @pl.loop(0, 2)
    @jax.named_scope('project')
    def _(u):
        for i in range(2):
            @pl.when(u == i)
            def _():
                weight_loads[1 + i].wait()

        res[...] = project(1 + u, far)

        @pl.when(u == 0)
        def _():
            keep_keys(far)
            for load in proj_loads:
                load.start()

        @pl.when(u == 1)
        def _():
            keep_values(far)

    with jax.named_scope('barrier'):
        pl.semaphore_wait(barrier, z.sp - 1 + z.sides)

    send_head(mirror(z.heads - 1 - inner))

    @pl.loop(2, 4 * z.slabs)
    @jax.named_scope('project')
    def _(u):
        early = u < 2 * z.slabs
        kind = jnp.where(early, 1 + u % 2, jnp.where(u < 3 * z.slabs, 0, 3))
        step = jnp.where(early, u // 2, u % z.slabs)
        slab = jnp.where(upper, step, z.slabs - 1 - step)

        @pl.when(u == 2 * z.slabs)
        def _():
            weight_loads[0].wait()

        @pl.when(u == 2)
        def _():
            weight_loads[3].wait()

            @pl.when(me < z.sp - 1)
            def _():
                rim_own[...] = jnp.dot(
                    tok[z.rows - REACH :], weights[3], preferred_element_type=f32).astype(bf16)
                rim_copy().start()

        cols = pl.ds(pl.multiple_of(slab * SLAB, SLAB), SLAB)
        res[...] = project(kind, slab)

        @pl.when(kind == 0)
        def _():
            for i in range(z.slab_heads):
                for t in range(z.tp):
                    for a in range(PASSES):
                        at = t * z.piece + a * z.run
                        to = (t % z.per) * z.run
                        q_own[slab * z.slab_heads + i, a, t // z.per, to : to + z.run] = (
                            res[at : at + z.run, i * VDIM : i * VDIM + VDIM] * (HEAD ** (-0.5) * log2_e)
                        ).astype(bf16)

            @pl.when(step == z.slabs - 1)
            def _():
                for a in range(PASSES):
                    q_all[a, me] = q_own[head, a, place]
                send_queries(0)

        @pl.when(kind == 1)
        def _():
            keep_keys(slab)

        @pl.when(kind == 2)
        def _():
            keep_values(slab)

            @pl.when(step == z.slabs - 1)
            def _():
                for h in range(half):
                    send_head(mirror(h))
                for j in range(half - 1):
                    send_head(other_far(j))

        @pl.when(kind == 3)
        def _():
            pool_in[:, cols] = res[...].astype(bf16)

    def relay(source):
        for kind in range(2):
            with jax.named_scope(f'zwait{kind}'):
                z_copy(kind, head, source * z.share + place).wait_recv()
            spread(kind, source)

    def relayed(j):
        if j == 0:
            return mirror(z.heads - 1 - inner)
        if j < half:
            return mirror(j - 1 + jnp.where(j - 1 >= inner, 1, 0))
        return other_far(j - half)

    @pl.when(me == 0)
    def _():
        rim[...] = jnp.zeros_like(rim)

    @pl.when(me > 0)
    def _():
        rim_copy().wait_recv()

    @pl.loop(0, z.width // 128)
    @jax.named_scope('pool')
    def _(pair):
        cols = pl.ds(pl.multiple_of(pair * 128, 128), 128)
        x = pool_in[:, cols].astype(f32)
        running = jnp.concatenate([rim[:, cols].astype(f32), x], 0)
        group = spot * (z.width // GDIM) + pair * 2 + lax.broadcasted_iota(jnp.int32, (1, 128), 1) // GDIM
        total = jnp.zeros_like(running)
        for level in range(4):
            running = running + pltpu.roll(running, 1 << level, 0)
            total = jnp.where(group % 4 == level, running, total)
        window = 2 << (group % 4)
        position = me * z.rows + lax.broadcasted_iota(jnp.int32, (z.rows, 1), 0)
        count = jnp.minimum(position + 1, window).astype(f32)
        pooled = (total[REACH:] / count - x).astype(bf16)
        mixed = jnp.dot(pooled, mix_ref[pair], preferred_element_type=f32)
        mixed = (mixed * scale_ref[:, cols]).astype(bf16)
        for t in range(z.tp):
            for a in range(PASSES):
                at = t * z.piece + a * z.run
                pool_out[a, t % 2, t // 2, :, cols] = mixed[at : at + z.run]

    for load in proj_loads:
        load.wait()

    flat = z.sides * z.run

    def term(left, a, part, at):
        cols = pl.ds(pl.multiple_of(part * SPAN, SPAN), SPAN)
        rows = jnp.concatenate(
            [left[a, c].reshape(flat, z.width) for c in (core, 1 - core)], 0)
        both = jnp.dot(rows, proj[at : at + z.width, cols], preferred_element_type=f32)
        return both[:flat].reshape(z.sides, z.run, SPAN), both[flat:].reshape(z.sides, z.run, SPAN)

    relay(relayed(0))

    @pl.loop(0, PASSES * z.parts)
    @jax.named_scope('poolproj')
    def _(i):
        a, part = i // z.parts, i % z.parts
        mine[a, part], theirs[a, part] = term(pool_out, a, part, 0)

    for j in range(1, z.heads - 1):
        relay(relayed(j))

    def lhs_at(a, source):
        p = source % z.share
        cols = pl.ds(pl.multiple_of((source // z.share) * VDIM, VDIM), VDIM)
        if z.per == 1:
            return lhs.at[a, p % 2, p // 2, :, cols]
        return lhs.at[a, :, p, :, cols]

    def o_copy(a, target, source):
        return to_sp(o_own.at[a, target], lhs_at(a, source), o_send.at[a, target], o_recv.at[a, source], target)

    def attend(a, duo):
        waiting = jax.named_scope('qwait')
        waiting.__enter__()
        for j in range(2):
            block = 2 * duo + j

            @pl.when(block != me)
            def _():
                q_copy(a, head, place, block).wait_recv()


        waiting.__exit__(None, None, None)
        lane = lax.broadcasted_iota(jnp.int32, (z.n, VDIM), 1)
        for j in range(2):
            query = q_all[a, 2 * duo + j]
            stacked[2 * j * z.n : (2 * j + 1) * z.n] = jnp.where(lane < HEAD, query, 0)
            stacked[(2 * j + 1) * z.n : (2 * j + 2) * z.n] = jnp.where(lane < HEAD, 0, query)
        turned[...] = stacked[...].T

        @pl.when(duo == 0)
        def _():
            key_seg = lax.broadcasted_iota(jnp.int32, (z.rows, 1), 0) // SEGMENT
            row = lax.broadcasted_iota(jnp.int32, (1, 2 * z.n), 1) % z.n
            token = (place * z.per + row // z.run) * z.piece + a * z.run + row % z.run
            bias[...] = jnp.where(key_seg <= token // SEGMENT, 0.0, neg_big)

        def put(buffer, block):
            value = jnp.dot(k_all[block], turned[...], preferred_element_type=f32)
            buffer[...] = value
            return jnp.max(value, axis=0, keepdims=True)

        def absorb(buffer, top, block, state):
            old, total = state
            new = jnp.maximum(old, top)
            shrink = jnp.exp2(old - new)
            probs = jnp.exp2(buffer[...] - new)
            total = total * shrink + jnp.sum(probs, axis=0, keepdims=True)
            acc[...] = acc[...] * shrink + jnp.dot(v_all[block], probs.astype(bf16), preferred_element_type=f32)
            return new, total

        split = 2 * z.n
        value = jnp.dot(k_all[2 * duo], turned[...], preferred_element_type=f32)
        low = value[:, :split] + bias[...]
        even[:, :split] = low
        even[:, split:] = value[:, split:]
        top = jnp.concatenate(
            [jnp.max(low, axis=0, keepdims=True), jnp.max(value[:, split:], axis=0, keepdims=True)], 1)
        high = jnp.dot(k_all[2 * duo + 1], turned[:, split:], preferred_element_type=f32) + bias[...]
        odd[:, split:] = high
        top_high = jnp.max(high, axis=0, keepdims=True)
        probs = jnp.exp2(even[...] - top)
        total = jnp.sum(probs, axis=0, keepdims=True)
        acc[...] = jnp.dot(v_all[2 * duo], probs.astype(bf16), preferred_element_type=f32)
        top_even = put(even, 0)
        new = jnp.maximum(top[:, split:], top_high)
        shrink = jnp.exp2(top[:, split:] - new)
        probs = jnp.exp2(odd[:, split:] - new)
        high = total[:, split:] * shrink + jnp.sum(probs, axis=0, keepdims=True)
        total = jnp.concatenate([total[:, :split], high], 1)
        top = jnp.concatenate([top[:, :split], new], 1)
        acc[:, split:] = acc[:, split:] * shrink + jnp.dot(
            v_all[2 * duo + 1], probs.astype(bf16), preferred_element_type=f32)

        def two(i, carry):
            state, top_even = carry
            top_odd = put(odd, 2 * i + 1)
            state = absorb(even, top_even, 2 * i, state)
            top_even = put(even, 2 * i + 2)
            state = absorb(odd, top_odd, 2 * i + 1, state)
            return state, top_even

        (_, total), _ = lax.fori_loop(0, duo, two, ((top, total), top_even))

        averaged = (acc[...] / total).T
        for j in range(2):
            block = 2 * duo + j
            one = averaged[2 * j * z.n : (2 * j + 1) * z.n]
            two_ = averaged[(2 * j + 1) * z.n : (2 * j + 2) * z.n]
            blend = one - lam_ref[head] * two_
            scaled = blend * lax.rsqrt(jnp.mean(blend * blend, axis=-1, keepdims=True) + eps_norm)
            scaled = (scaled * head_gain_ref[...] * out_scale).astype(bf16)
            o_own[a, block] = scaled if z.per == 1 else scaled.reshape(z.per, z.run, VDIM)

            @pl.when(block == me)
            def _():
                lhs_at(a, me)[...] = o_own[a, block]

            @pl.when(block != me)
            def _():
                o_copy(a, block, me).start()

    def pair_copy(a, part):
        return to_tp(pairs_out.at[a, part], pairs_in.at[a, part], pair_send.at[a, part], pair_recv.at[a, part], mate)

    def far_copy(a, away, part):
        other = ((side + away) % z.sides) * 2 + core
        return to_tp(far_out.at[a, away, part], far_in.at[a, away, part], far_send.at[a, away, part],
                     far_recv.at[a, away, part], other)

    def merge(a):
        with jax.named_scope('owait'):
            @pl.loop(1, z.sp)
            def _(away):
                o_copy(a, me, (me + away) % z.sp).wait_recv()

        @pl.loop(0, z.parts + LAG)
        def _(part):
            @pl.when(part < z.parts)
            def _():
                ours, others = term(lhs, a, part, z.width)
                mine[a, part] = mine[a, part] + ours
                pairs_out[a, part] = (theirs[a, part] + others).astype(bf16)
                pair_copy(a, part).start()

            @pl.when(part >= LAG)
            def _():
                last = part - LAG
                pair_copy(a, last).wait_recv()
                for away in range(1, z.sides):
                    s = (side + away) % z.sides
                    far_out[a, away, last] = (mine[a, last, s] + pairs_in[a, last, s].astype(f32)).astype(bf16)
                    far_copy(a, away, last).start()
                mine[a, last, side] = mine[a, last, side] + pairs_in[a, last, side].astype(f32)

    duos = z.sp // 2
    per_head = z.share // 2
    last = PASSES * duos

    @pl.loop(0, last + 1)
    def _(it):
        pass_ = (it - HOLD) // duos

        @pl.when(((it >= duos + HOLD) & ((it - HOLD) % duos == 0) & (it < last)) | (it == last))
        @jax.named_scope('merge')
        def _():
            merge(jnp.where(it == last, PASSES - 1, pass_ - 1))

        @pl.when((it < duos) & (it % per_head == 0))
        @jax.named_scope('relay')
        def _():
            source = it // per_head

            @pl.loop(1, z.share)
            def _(away):
                for kind in range(2):
                    with jax.named_scope(f'xwait{kind}'):
                        x_copy(kind, source, source * z.share + (place + away) % z.share, place).wait_recv()

        @pl.when((it % duos == ASK) & (it < PASSES * duos - duos))
        def _():
            send_queries(it // duos + 1)

        @pl.when(it < PASSES * duos)
        @jax.named_scope('attend')
        def _():
            attend(it // duos, it % duos)

    @pl.loop(0, PASSES * z.parts)
    @jax.named_scope('final')
    def _(i):
        a, part = i // z.parts, i % z.parts
        total = mine[a, part, side]
        for away in range(1, z.sides):
            far_copy(a, away, part).wait_recv()
            total = total + far_in[a, away, part].astype(f32)
        at = pl.ds(pl.multiple_of(a * z.run, z.run), z.run)
        out_ref[at, pl.ds(pl.multiple_of(part * SPAN, SPAN), SPAN)] = total.astype(bf16)

    for kind in range(2):
        for away in range(1, z.heads):
            z_copy(kind, (head + away) % z.heads, me).wait_send()
        for h in range(z.heads):
            for away in range(1, z.share):
                x_copy(kind, h, h * z.share + place, (place + away) % z.share).wait_send()
    for a in range(PASSES):
        @pl.loop(1, z.sp)
        def _(away):
            target = (me + away) % z.sp
            q_copy(a, target // z.share, target % z.share, me).wait_send()
            o_copy(a, target, me).wait_send()

        @pl.loop(0, z.parts)
        def _(part):
            pair_copy(a, part).wait_send()
            for away in range(1, z.sides):
                far_copy(a, away, part).wait_send()

    @pl.when(me < z.sp - 1)
    def _():
        rim_copy().wait_send()


def body(tokens, norm_gain, w_pool_in, w_query, w_key, w_value, pool_mix, pool_scale, lam, head_gain, pool_proj,
         attn_proj):
    rows, depth = tokens.shape
    width = w_query.shape[1]
    z = Shape(lax.axis_size("sp"), lax.axis_size("tp"), rows, depth, width)
    pairs = pool_mix.reshape(-1, 2, GDIM, GDIM)
    zero = jnp.zeros_like(pairs[:, 0])
    mix = jnp.concatenate(
        [jnp.concatenate([pairs[:, 0], zero], 2), jnp.concatenate([zero, pairs[:, 1]], 2)], 1)
    vmem = pl.BlockSpec(memory_space=pltpu.VMEM)
    hbm = pl.BlockSpec(memory_space=pl.ANY)
    bf16, f32 = jnp.bfloat16, jnp.float32
    dma = pltpu.SemaphoreType.DMA
    scratch = [
        pltpu.VMEM((rows, depth), bf16),
        pltpu.VMEM((4, depth, width), bf16),
        pltpu.VMEM((2 * width, depth), bf16),
        pltpu.VMEM((rows, SLAB), f32),
        pltpu.VMEM((z.heads, rows, VDIM), bf16),
        pltpu.VMEM((z.heads, VDIM, rows), bf16),
        pltpu.VMEM((z.heads, PASSES, z.share, z.n, VDIM), bf16),
        pltpu.VMEM((z.sp, rows, VDIM), bf16),
        pltpu.VMEM((z.sp, VDIM, rows), bf16),
        pltpu.VMEM((PASSES, z.sp, z.n, VDIM), bf16),
        pltpu.VMEM((PASSES, 2, z.sides, z.run, width), bf16),
        pltpu.VMEM((PASSES, 2, z.sides, z.run, width), bf16),
        pltpu.VMEM((PASSES, z.sp) + ((z.n,) if z.per == 1 else (z.per, z.run)) + (VDIM,), bf16),
        pltpu.VMEM((rows, width), bf16),
        pltpu.VMEM((REACH, width), bf16),
        pltpu.VMEM((REACH, width), bf16),
        pltpu.VMEM((z.cols, VDIM), bf16),
        pltpu.VMEM((VDIM, z.cols), bf16),
        pltpu.VMEM((rows, z.cols), f32),
        pltpu.VMEM((rows, z.cols), f32),
        pltpu.VMEM((rows, 2 * z.n), f32),
        pltpu.VMEM((VDIM, z.cols), f32),
        pltpu.VMEM((PASSES, z.parts, z.sides, z.run, SPAN), bf16),
        pltpu.VMEM((PASSES, z.parts, z.sides, z.run, SPAN), bf16),
        pltpu.VMEM((PASSES, z.parts, z.sides, z.run, SPAN), f32),
        pltpu.VMEM((PASSES, z.parts, z.sides, z.run, SPAN), f32),
        pltpu.VMEM((PASSES, z.sides, z.parts, z.run, SPAN), bf16),
        pltpu.VMEM((PASSES, z.sides, z.parts, z.run, SPAN), bf16),
        dma((LOADS,)), dma((4,)), dma((2,)),
        dma((2, z.heads)), dma((2, z.heads)),
        dma((2, z.heads, z.share)), dma((2, z.heads, z.share)),
        dma((PASSES, z.sp)), dma((PASSES, z.sp)),
        dma((PASSES, z.sp)), dma((PASSES, z.sp)),
        dma, dma,
        dma((PASSES, z.parts)), dma((PASSES, z.parts)),
        dma((PASSES, z.sides, z.parts)), dma((PASSES, z.sides, z.parts)),
    ]
    return pl.pallas_call(
        functools.partial(layer_kernel, z),
        out_shape=jax.ShapeDtypeStruct((rows // z.tp, depth), bf16),
        in_specs=[pl.BlockSpec(memory_space=pltpu.SMEM), hbm, vmem, hbm, hbm, hbm, hbm, vmem, vmem, vmem, hbm, hbm],
        out_specs=vmem,
        scratch_shapes=scratch,
        compiler_params=pltpu.CompilerParams(
            collective_id=0, has_side_effects=True, vmem_limit_bytes=57 * 2**20),
        name="layer",
    )(lam, tokens, norm_gain.reshape(1, depth), w_pool_in, w_query, w_key, w_value, mix,
      pool_scale.reshape(1, width), head_gain.reshape(1, VDIM), pool_proj, attn_proj)


def solution(mesh):
    return jax.shard_map(
        body,
        mesh=mesh,
        in_specs=(
            P("sp", None), P(), P(None, "tp"), P(None, "tp"), P(None, "tp"), P(None, "tp"),
            P("tp", None, None), P("tp"), P("tp"), P(), P("tp", None), P("tp", None),
        ),
        out_specs=P(("sp", "tp"), None),
        check_vma=False,
    )
```

```python
import functools

import jax
import jax.numpy as jnp
from jax import lax
from jax.experimental import pallas as pl
from jax.experimental.pallas import tpu as pltpu
from jax.sharding import PartitionSpec as P

GDIM = 64
HEAD = 64
VDIM = 128
SEGMENT = 64
REACH = 16
PASSES = 2
SPAN = 1024
SLAB = 256
HOLDS = (2, 2, 2, 2)
ASK = 2
LAG = 2
BAND = 64
LOADS = 4
MESH = pl.DeviceIdType.MESH

eps_norm = 1e-06
neg_big = -1e30
out_scale = 0.8
log2_e = 1.4426950408889634


class Shape:
    def __init__(self, sp, tp, rows, depth, width):
        self.sp, self.tp, self.rows, self.depth, self.width = sp, tp, rows, depth, width
        self.heads = width // VDIM
        self.share = sp // self.heads
        self.per = tp // self.share
        assert self.per in (1, 2) and self.share % 2 == 0
        self.piece = rows // tp
        self.run = self.piece // PASSES
        self.n = self.per * self.run
        self.cols = 4 * self.n
        self.sides = tp // 2
        self.parts = depth // SPAN
        self.slabs = width // SLAB
        self.slab_heads = SLAB // VDIM


def layer_kernel(z, lam_ref, tok_hbm, gain_ref, wp_hbm, wq_hbm, wk_hbm, wv_hbm, mix_ref, scale_ref, head_gain_ref,
                 pp_hbm, ap_hbm, out_ref,
                 tok, weights, proj, res, k_own, v_own, q_own, k_all, v_all, q_all, pool_out, lhs, o_own, pool_in, rim, rim_own,
                 stacked, turned, even, odd, bias, acc, pairs_out, pairs_in, mine, theirs, far_out, far_in, ready,
                 tok_sem, w_sem, p_sem, z_send, z_recv, x_send, x_recv, q_send, q_recv, o_send, o_recv,
                 rim_send, rim_recv, pair_send, pair_recv, far_send, far_recv, store_sem):
    me = lax.axis_index("sp")
    spot = lax.axis_index("tp")
    head, place = me // z.share, me % z.share
    side, core = spot // 2, spot % 2
    mate = side * 2 + 1 - core
    bf16, f32 = jnp.bfloat16, jnp.float32

    def to_sp(src, dst, send, recv, device):
        return pltpu.make_async_remote_copy(
            src_ref=src, dst_ref=dst, send_sem=send, recv_sem=recv,
            device_id={"sp": device}, device_id_type=MESH)

    def to_tp(src, dst, send, recv, device):
        return pltpu.make_async_remote_copy(
            src_ref=src, dst_ref=dst, send_sem=send, recv_sem=recv,
            device_id={"tp": device}, device_id_type=MESH)

    chunk = z.rows // LOADS

    def token_load(i):
        at = pl.ds(pl.multiple_of(i * chunk, chunk), chunk)
        return pltpu.make_async_copy(tok_hbm.at[at], tok.at[at], tok_sem.at[i])

    weight_loads = [
        pltpu.make_async_copy(w, weights.at[i], w_sem.at[i])
        for i, w in enumerate((wq_hbm, wk_hbm, wv_hbm, wp_hbm))
    ]
    proj_loads = [
        pltpu.make_async_copy(w, proj.at[pl.ds(i * z.width, z.width)], p_sem.at[i])
        for i, w in enumerate((pp_hbm, ap_hbm))
    ]
    for i in range(LOADS):
        token_load(i).start()

    barrier = pltpu.get_barrier_semaphore()
    for away in range(1, z.sp):
        pl.semaphore_signal(barrier, inc=1, device_id={"sp": (me + away) % z.sp}, device_id_type=MESH)
    pl.semaphore_signal(barrier, inc=1, device_id={"tp": mate}, device_id_type=MESH)
    for away in range(1, z.sides):
        other = ((side + away) % z.sides) * 2 + core
        pl.semaphore_signal(barrier, inc=1, device_id={"tp": other}, device_id_type=MESH)

    @pl.loop(0, LOADS)
    @jax.named_scope('norm')
    def _(i):
        token_load(i).wait()
        for at in range(4):
            @pl.when(i == (3, 0, 2, 3)[at])
            def _():
                weight_loads[at].start()

        @pl.loop(0, chunk // BAND)
        def _(j):
            at = pl.ds(pl.multiple_of(i * chunk + j * BAND, BAND), BAND)
            total = jnp.zeros((BAND, 128), f32)
            for c in range(0, z.depth, 128):
                wide = tok[at, c : c + 128].astype(f32)
                total = total + wide * wide
            scale = lax.rsqrt(jnp.sum(total, axis=-1, keepdims=True) * (1.0 / z.depth) + eps_norm)
            scale = jnp.broadcast_to(scale, (BAND, 128))
            for c in range(0, z.depth, 128):
                wide = tok[at, c : c + 128].astype(f32)
                tok[at, c : c + 128] = (wide * scale * gain_ref[:, c : c + 128]).astype(bf16)

    def z_copy(kind, h, source):
        own, all_ = ((k_own, k_all), (v_own, v_all))[kind]
        return to_sp(own.at[h], all_.at[source], z_send.at[kind, h], z_recv.at[kind, source // z.share],
                     h * z.share + place)

    def x_copy(kind, h, source, target):
        all_ = (k_all, v_all)[kind]
        return to_sp(all_.at[source], all_.at[source], x_send.at[kind, h, target],
                     x_recv.at[kind, h, source % z.share], head * z.share + target)

    def spread(kind, h):
        for away in range(1, z.share):
            x_copy(kind, h, h * z.share + place, (place + away) % z.share).start()

    def send_head(h):
        @pl.when(h == head)
        def _():
            k_all[me] = k_own[h]
            v_all[me] = v_own[h]
            for kind in range(2):
                spread(kind, h)

        @pl.when(h != head)
        def _():
            for kind in range(2):
                z_copy(kind, h, me).start()

    def q_copy(a, h, p, source):
        target = h * z.share + p
        return to_sp(q_own.at[h, a, p], q_all.at[a, source], q_send.at[a, target], q_recv.at[a, source], target)

    def send_queries(a):
        @pl.loop(1, z.sp)
        def _(away):
            target = (me + away) % z.sp
            q_copy(a, target // z.share, target % z.share, me).start()

    def rim_copy():
        return to_sp(rim_own, rim, rim_send, rim_recv, (me + 1) % z.sp)

    upper = head >= z.heads // 2

    def project(kind, slab):
        cols = pl.ds(pl.multiple_of(slab * SLAB, SLAB), SLAB)
        return jnp.dot(tok[...], weights[kind, :, cols], preferred_element_type=f32)

    def keep_keys(slab):
        for i in range(z.slab_heads):
            k_own[slab * z.slab_heads + i] = res[:, i * VDIM : i * VDIM + VDIM].astype(bf16)

    def keep_values(slab):
        for i in range(z.slab_heads):
            v_own[slab * z.slab_heads + i] = res[:, i * VDIM : i * VDIM + VDIM].astype(bf16).T

    half = z.heads // 2

    def mirror(h):
        return jnp.where(upper, z.heads - 1 - h, h)

    inner = mirror(head)

    def other_far(j):
        return mirror(half + j + jnp.where(half + j >= z.heads - 1 - inner, 1, 0))

    def send_rest():
        for h in range(half):
            send_head(mirror(h))
        for j in range(half - 1):
            send_head(other_far(j))

    far = jnp.where(upper, 0, z.slabs - 1)

    @pl.loop(0, 2)
    @jax.named_scope('project')
    def _(u):
        for i in range(2):
            @pl.when(u == i)
            def _():
                weight_loads[1 + i].wait()

        res[...] = project(1 + u, far)

        @pl.when(u == 0)
        def _():
            keep_keys(far)
            for load in proj_loads:
                load.start()

        @pl.when(u == 1)
        def _():
            keep_values(far)

    with jax.named_scope('barrier'):
        pl.semaphore_wait(barrier, z.sp - 1 + z.sides)

    send_head(mirror(z.heads - 1 - inner))
    if z.slabs == 1:
        send_rest()

    @pl.loop(2, 4 * z.slabs)
    @jax.named_scope('project')
    def _(u):
        early = u < 2 * z.slabs
        kind = jnp.where(early, 1 + u % 2, jnp.where(u < 3 * z.slabs, 0, 3))
        step = jnp.where(early, u // 2, u % z.slabs)
        slab = jnp.where(upper, step, z.slabs - 1 - step)

        @pl.when(u == 2 * z.slabs)
        def _():
            weight_loads[0].wait()

        @pl.when(u == 2)
        def _():
            weight_loads[3].wait()

            @pl.when(me < z.sp - 1)
            def _():
                rim_own[...] = jnp.dot(
                    tok[z.rows - REACH :], weights[3], preferred_element_type=f32).astype(bf16)
                rim_copy().start()

        cols = pl.ds(pl.multiple_of(slab * SLAB, SLAB), SLAB)
        res[...] = project(kind, slab)

        @pl.when(kind == 0)
        def _():
            for i in range(z.slab_heads):
                for t in range(z.tp):
                    for a in range(PASSES):
                        at = t * z.piece + a * z.run
                        to = (t % z.per) * z.run
                        q_own[slab * z.slab_heads + i, a, t // z.per, to : to + z.run] = (
                            res[at : at + z.run, i * VDIM : i * VDIM + VDIM] * (HEAD ** (-0.5) * log2_e)
                        ).astype(bf16)

            @pl.when(step == z.slabs - 1)
            def _():
                for a in range(PASSES):
                    q_all[a, me] = q_own[head, a, place]
                send_queries(0)

        @pl.when(kind == 1)
        def _():
            keep_keys(slab)

        @pl.when(kind == 2)
        def _():
            keep_values(slab)

            @pl.when(step == z.slabs - 1)
            def _():
                send_rest()

        @pl.when(kind == 3)
        def _():
            pool_in[:, cols] = res[...].astype(bf16)

    def relay(source):
        for kind in range(2):
            with jax.named_scope(f'zwait{kind}'):
                z_copy(kind, head, source * z.share + place).wait_recv()
            spread(kind, source)

    def relayed(j):
        if j == 0:
            return mirror(z.heads - 1 - inner)
        if j < half:
            return mirror(j - 1 + jnp.where(j - 1 >= inner, 1, 0))
        return other_far(j - half)

    @pl.when(me == 0)
    def _():
        rim[...] = jnp.zeros_like(rim)

    @pl.when(me > 0)
    def _():
        rim_copy().wait_recv()

    @pl.loop(0, z.width // 128)
    @jax.named_scope('pool')
    def _(pair):
        cols = pl.ds(pl.multiple_of(pair * 128, 128), 128)
        x = pool_in[:, cols].astype(f32)
        running = jnp.concatenate([rim[:, cols].astype(f32), x], 0)
        group = spot * (z.width // GDIM) + pair * 2 + lax.broadcasted_iota(jnp.int32, (1, 128), 1) // GDIM
        total = jnp.zeros_like(running)
        for level in range(4):
            running = running + pltpu.roll(running, 1 << level, 0)
            total = jnp.where(group % 4 == level, running, total)
        window = 2 << (group % 4)
        position = me * z.rows + lax.broadcasted_iota(jnp.int32, (z.rows, 1), 0)
        count = jnp.minimum(position + 1, window).astype(f32)
        pooled = (total[REACH:] / count - x).astype(bf16)
        wide = lax.broadcasted_iota(jnp.int32, (GDIM, 128), 1) - lax.broadcasted_iota(jnp.int32, (GDIM, 128), 0)
        mix = jnp.concatenate(
            [jnp.dot(mix_ref[2 * pair + j], (wide == j * GDIM).astype(bf16), preferred_element_type=f32).astype(bf16)
             for j in range(2)], 0)
        mixed = jnp.dot(pooled, mix, preferred_element_type=f32)
        mixed = (mixed * scale_ref[:, cols]).astype(bf16)
        for t in range(z.tp):
            for a in range(PASSES):
                at = t * z.piece + a * z.run
                pool_out[a, t % 2, t // 2, :, cols] = mixed[at : at + z.run]

    for load in proj_loads:
        load.wait()

    flat = z.sides * z.run

    def term(left, a, part, at):
        cols = pl.ds(pl.multiple_of(part * SPAN, SPAN), SPAN)
        rows = jnp.concatenate(
            [left[a, c].reshape(flat, z.width) for c in (core, 1 - core)], 0)
        both = jnp.dot(rows, proj[at : at + z.width, cols], preferred_element_type=f32)
        return both[:flat].reshape(z.sides, z.run, SPAN), both[flat:].reshape(z.sides, z.run, SPAN)

    relay(relayed(0))

    @pl.loop(0, PASSES * z.parts)
    @jax.named_scope('poolproj')
    def _(i):
        a, part = i // z.parts, i % z.parts
        mine[a, part], theirs[a, part] = term(pool_out, a, part, 0)

    for j in range(1, z.heads - 1):
        relay(relayed(j))

    def lhs_at(a, source):
        p = source % z.share
        cols = pl.ds(pl.multiple_of((source // z.share) * VDIM, VDIM), VDIM)
        if z.per == 1:
            return lhs.at[a, p % 2, p // 2, :, cols]
        return lhs.at[a, :, p, :, cols]

    def o_copy(a, target, source):
        return to_sp(o_own.at[a, target], lhs_at(a, source), o_send.at[a, target], o_recv.at[a, source], target)

    def attend(a, duo):
        waiting = jax.named_scope('qwait')
        waiting.__enter__()
        for j in range(2):
            block = 2 * duo + j

            @pl.when(block != me)
            def _():
                q_copy(a, head, place, block).wait_recv()


        waiting.__exit__(None, None, None)
        lane = lax.broadcasted_iota(jnp.int32, (z.n, VDIM), 1)
        for j in range(2):
            query = q_all[a, 2 * duo + j]
            stacked[2 * j * z.n : (2 * j + 1) * z.n] = jnp.where(lane < HEAD, query, 0)
            stacked[(2 * j + 1) * z.n : (2 * j + 2) * z.n] = jnp.where(lane < HEAD, 0, query)
        turned[...] = stacked[...].T

        @pl.when(duo == 0)
        def _():
            key_seg = lax.broadcasted_iota(jnp.int32, (z.rows, 1), 0) // SEGMENT
            row = lax.broadcasted_iota(jnp.int32, (1, 2 * z.n), 1) % z.n
            token = (place * z.per + row // z.run) * z.piece + a * z.run + row % z.run
            bias[...] = jnp.where(key_seg <= token // SEGMENT, 0.0, neg_big)

        def put(buffer, block):
            value = jnp.dot(k_all[block], turned[...], preferred_element_type=f32)
            buffer[...] = value
            return jnp.max(value, axis=0, keepdims=True)

        def absorb(buffer, top, block, state):
            old, total = state
            new = jnp.maximum(old, top)
            shrink = jnp.exp2(old - new)
            probs = jnp.exp2(buffer[...] - new)
            total = total * shrink + jnp.sum(probs, axis=0, keepdims=True)
            acc[...] = acc[...] * shrink + jnp.dot(v_all[block], probs.astype(bf16), preferred_element_type=f32)
            return new, total

        split = 2 * z.n
        value = jnp.dot(k_all[2 * duo], turned[...], preferred_element_type=f32)
        low = value[:, :split] + bias[...]
        even[:, :split] = low
        even[:, split:] = value[:, split:]
        top = jnp.concatenate(
            [jnp.max(low, axis=0, keepdims=True), jnp.max(value[:, split:], axis=0, keepdims=True)], 1)
        high = jnp.dot(k_all[2 * duo + 1], turned[:, split:], preferred_element_type=f32) + bias[...]
        odd[:, split:] = high
        top_high = jnp.max(high, axis=0, keepdims=True)
        probs = jnp.exp2(even[...] - top)
        total = jnp.sum(probs, axis=0, keepdims=True)
        acc[...] = jnp.dot(v_all[2 * duo], probs.astype(bf16), preferred_element_type=f32)
        top_even = put(even, 0)
        new = jnp.maximum(top[:, split:], top_high)
        shrink = jnp.exp2(top[:, split:] - new)
        probs = jnp.exp2(odd[:, split:] - new)
        high = total[:, split:] * shrink + jnp.sum(probs, axis=0, keepdims=True)
        total = jnp.concatenate([total[:, :split], high], 1)
        top = jnp.concatenate([top[:, :split], new], 1)
        acc[:, split:] = acc[:, split:] * shrink + jnp.dot(
            v_all[2 * duo + 1], probs.astype(bf16), preferred_element_type=f32)

        def two(i, carry):
            state, top_even = carry
            top_odd = put(odd, 2 * i + 1)
            state = absorb(even, top_even, 2 * i, state)
            top_even = put(even, 2 * i + 2)
            state = absorb(odd, top_odd, 2 * i + 1, state)
            return state, top_even

        (_, total), _ = lax.fori_loop(0, duo, two, ((top, total), top_even))

        averaged = (acc[...] / total).T
        for j in range(2):
            block = 2 * duo + j
            one = averaged[2 * j * z.n : (2 * j + 1) * z.n]
            two_ = averaged[(2 * j + 1) * z.n : (2 * j + 2) * z.n]
            blend = one - lam_ref[head] * two_
            scaled = blend * lax.rsqrt(jnp.mean(blend * blend, axis=-1, keepdims=True) + eps_norm)
            scaled = (scaled * head_gain_ref[...] * out_scale).astype(bf16)
            o_own[a, block] = scaled if z.per == 1 else scaled.reshape(z.per, z.run, VDIM)

            @pl.when(block == me)
            def _():
                lhs_at(a, me)[...] = o_own[a, block]

            @pl.when(block != me)
            def _():
                o_copy(a, block, me).start()

    def pair_copy(a, part):
        return to_tp(pairs_out.at[a, part], pairs_in.at[a, part], pair_send.at[a, part], pair_recv.at[a, part], mate)

    def far_copy(a, away, part):
        other = ((side + away) % z.sides) * 2 + core
        return to_tp(far_out.at[a, away, part], far_in.at[a, away, part], far_send.at[a, away, part],
                     far_recv.at[a, away, part], other)

    def merge(a):
        with jax.named_scope('owait'):
            @pl.loop(1, z.sp)
            def _(away):
                o_copy(a, me, (me + away) % z.sp).wait_recv()

        @pl.loop(0, z.parts + LAG)
        def _(part):
            @pl.when(part < z.parts)
            def _():
                ours, others = term(lhs, a, part, z.width)
                mine[a, part] = mine[a, part] + ours
                pairs_out[a, part] = (theirs[a, part] + others).astype(bf16)
                pair_copy(a, part).start()

            @pl.when(part >= LAG)
            def _():
                last = part - LAG
                pair_copy(a, last).wait_recv()
                for away in range(1, z.sides):
                    s = (side + away) % z.sides
                    far_out[a, away, last] = (mine[a, last, s] + pairs_in[a, last, s].astype(f32)).astype(bf16)
                    far_copy(a, away, last).start()
                mine[a, last, side] = mine[a, last, side] + pairs_in[a, last, side].astype(f32)

    duos = z.sp // 2
    per_head = z.share // 2
    last = PASSES * duos

    hold = jnp.int32(HOLDS[0])
    for i in range(1, len(HOLDS)):
        hold = jnp.where(head * len(HOLDS) // z.heads == i, HOLDS[i], hold)
    hold = hold * duos // len(HOLDS)

    @pl.loop(0, last + 2)
    def _(it):
        @pl.when((it == duos + hold) | (it == last + 1))
        @jax.named_scope('merge')
        def _():
            merge(jnp.where(it == last + 1, 1, 0))

        @pl.when((it < duos) & (it % per_head == 0))
        @jax.named_scope('relay')
        def _():
            source = it // per_head

            @pl.loop(1, z.share)
            def _(away):
                for kind in range(2):
                    with jax.named_scope(f'xwait{kind}'):
                        x_copy(kind, source, source * z.share + (place + away) % z.share, place).wait_recv()

        @pl.when((it % duos == ASK) & (it < PASSES * duos - duos))
        def _():
            send_queries(it // duos + 1)

        @pl.when(it < PASSES * duos)
        @jax.named_scope('attend')
        def _():
            attend(it // duos, it % duos)

    for kind in range(2):
        for away in range(1, z.heads):
            z_copy(kind, (head + away) % z.heads, me).wait_send()
        for h in range(z.heads):
            for away in range(1, z.share):
                x_copy(kind, h, h * z.share + place, (place + away) % z.share).wait_send()
    for a in range(PASSES):
        @pl.loop(1, z.sp)
        def _(away):
            target = (me + away) % z.sp
            q_copy(a, target // z.share, target % z.share, me).wait_send()
            o_copy(a, target, me).wait_send()

        @pl.loop(0, z.parts)
        def _(part):
            pair_copy(a, part).wait_send()

    @pl.when(me < z.sp - 1)
    def _():
        rim_copy().wait_send()

    def store(a, part):
        at = pl.ds(pl.multiple_of(a * z.run, z.run), z.run)
        cols = pl.ds(pl.multiple_of(part * SPAN, SPAN), SPAN)
        return pltpu.make_async_copy(ready.at[a, part], out_ref.at[at, cols], store_sem.at[a, part])

    @pl.loop(0, PASSES * z.parts)
    @jax.named_scope('final')
    def _(i):
        a, part = i // z.parts, i % z.parts
        total = mine[a, part, side]
        for away in range(1, z.sides):
            far_copy(a, away, part).wait_recv()
            far_copy(a, away, part).wait_send()
            total = total + far_in[a, away, part].astype(f32)
        ready[a, part] = total.astype(bf16)
        store(a, part).start()

    @pl.loop(0, PASSES * z.parts)
    def _(i):
        store(i // z.parts, i % z.parts).wait()


def body(tokens, norm_gain, w_pool_in, w_query, w_key, w_value, pool_mix, pool_scale, lam, head_gain, pool_proj,
         attn_proj):
    rows, depth = tokens.shape
    width = w_query.shape[1]
    z = Shape(lax.axis_size("sp"), lax.axis_size("tp"), rows, depth, width)
    vmem = pl.BlockSpec(memory_space=pltpu.VMEM)
    hbm = pl.BlockSpec(memory_space=pl.ANY)
    bf16, f32 = jnp.bfloat16, jnp.float32
    dma = pltpu.SemaphoreType.DMA
    scratch = [
        pltpu.VMEM((rows, depth), bf16),
        pltpu.VMEM((4, depth, width), bf16),
        pltpu.VMEM((2 * width, depth), bf16),
        pltpu.VMEM((rows, SLAB), f32),
        pltpu.VMEM((z.heads, rows, VDIM), bf16),
        pltpu.VMEM((z.heads, VDIM, rows), bf16),
        pltpu.VMEM((z.heads, PASSES, z.share, z.n, VDIM), bf16),
        pltpu.VMEM((z.sp, rows, VDIM), bf16),
        pltpu.VMEM((z.sp, VDIM, rows), bf16),
        pltpu.VMEM((PASSES, z.sp, z.n, VDIM), bf16),
        pltpu.VMEM((PASSES, 2, z.sides, z.run, width), bf16),
        pltpu.VMEM((PASSES, 2, z.sides, z.run, width), bf16),
        pltpu.VMEM((PASSES, z.sp) + ((z.n,) if z.per == 1 else (z.per, z.run)) + (VDIM,), bf16),
        pltpu.VMEM((rows, width), bf16),
        pltpu.VMEM((REACH, width), bf16),
        pltpu.VMEM((REACH, width), bf16),
        pltpu.VMEM((z.cols, VDIM), bf16),
        pltpu.VMEM((VDIM, z.cols), bf16),
        pltpu.VMEM((rows, z.cols), f32),
        pltpu.VMEM((rows, z.cols), f32),
        pltpu.VMEM((rows, 2 * z.n), f32),
        pltpu.VMEM((VDIM, z.cols), f32),
        pltpu.VMEM((PASSES, z.parts, z.sides, z.run, SPAN), bf16),
        pltpu.VMEM((PASSES, z.parts, z.sides, z.run, SPAN), bf16),
        pltpu.VMEM((PASSES, z.parts, z.sides, z.run, SPAN), f32),
        pltpu.VMEM((PASSES, z.parts, z.sides, z.run, SPAN), f32),
        pltpu.VMEM((PASSES, z.sides, z.parts, z.run, SPAN), bf16),
        pltpu.VMEM((PASSES, z.sides, z.parts, z.run, SPAN), bf16),
        pltpu.VMEM((PASSES, z.parts, z.run, SPAN), bf16),
        dma((LOADS,)), dma((4,)), dma((2,)),
        dma((2, z.heads)), dma((2, z.heads)),
        dma((2, z.heads, z.share)), dma((2, z.heads, z.share)),
        dma((PASSES, z.sp)), dma((PASSES, z.sp)),
        dma((PASSES, z.sp)), dma((PASSES, z.sp)),
        dma, dma,
        dma((PASSES, z.parts)), dma((PASSES, z.parts)),
        dma((PASSES, z.sides, z.parts)), dma((PASSES, z.sides, z.parts)),
        dma((PASSES, z.parts)),
    ]
    return pl.pallas_call(
        functools.partial(layer_kernel, z),
        out_shape=jax.ShapeDtypeStruct((rows // z.tp, depth), bf16),
        in_specs=[pl.BlockSpec(memory_space=pltpu.SMEM), hbm, vmem, hbm, hbm, hbm, hbm, vmem, vmem, vmem, hbm, hbm],
        out_specs=hbm,
        scratch_shapes=scratch,
        compiler_params=pltpu.CompilerParams(
            collective_id=0, has_side_effects=True, vmem_limit_bytes=57 * 2**20),
        name="layer",
    )(lam, tokens, norm_gain.reshape(1, depth), w_pool_in, w_query, w_key, w_value, pool_mix,
      pool_scale.reshape(1, width), head_gain.reshape(1, VDIM), pool_proj, attn_proj)


def solution(mesh):
    return jax.shard_map(
        body,
        mesh=mesh,
        in_specs=(
            P("sp", None), P(), P(None, "tp"), P(None, "tp"), P(None, "tp"), P(None, "tp"),
            P("tp", None, None), P("tp"), P("tp"), P(), P("tp", None), P("tp", None),
        ),
        out_specs=P(("sp", "tp"), None),
        check_vma=False,
    )
```
